32 devices in a mesh: sp: 8 (over z, y), tp: 4 (over x, core).
Axes of the slice: x: 2, y: 2, z: 4, core: 2. Of those that a mesh axis runs over, the one named last changes fastest.
Arguments:
- stream: bfloat16 [16384, 4096], P('sp', 'tp'), may hold values from -18 to 18
- doc_ids: int32 [16384], P('sp'), may hold values from 0 to 1, never falling along the last dimension, each value on 1 to 12288 neighbouring positions
- norm_gain: bfloat16 [3, 4096], replicated, may hold values from 0.099609375 to 1.8984375
- proj_in: bfloat16 [3, 4096, 1024], P(None, 'tp', 'sp'), may hold values from -0.09375 to 0.09375
- mix_pool: bfloat16 [3, 8, 128, 128], replicated, may hold values from -0.5 to 0.5
- pool_gain: bfloat16 [3, 1024], replicated, may hold values from 0.099609375 to 1.8984375
- proj_out: bfloat16 [3, 1024, 4096], P(None, 'sp', 'tp'), may hold values from -0.1875 to 0.1875
Outputs:
- stream_out: bfloat16 [16384, 4096], P('sp', 'tp')
The draws below stay inside these ranges and needn't reach their ends.
Inputs may be any that keep to these rules, and one draw needn't show every extreme that they name: `doc_ids`: document numbers never fall along the sequence; each document holds 1 to 12288 positions, one exactly that many.
All inputs are finite; a program needn't handle non-finite values.
Results may differ from the reference program's by a relative error of at most 0.02.
Values may be sent and summed in bfloat16 or wider, within the bound.
A program may use at most 64 MiB of HBM per device.

```python
import math
import jax
import jax.numpy as jnp
import numpy as np
from jax import lax

D = 4096
POOL = 1024
GROUP = 128
LAYERS = 3
TOK = 2048
GROUPS = 8
TOKENS = 16384
DOCS = 2
N_TP = 4


def draw_stream(key, part):
    key_base = jax.random.fold_in(key, 11)
    key_cols = jax.random.fold_in(key, 12)
    column_scale = jnp.exp(jax.random.uniform(key_cols, (32,), jnp.float32, -1.1, 1.1))
    column_scale = jnp.repeat(column_scale, D // 32)
    base = jnp.clip(jax.random.normal(key_base, (TOKENS, D), jnp.float32), -6.0, 6.0)
    values = jnp.clip(base * column_scale[None, :], -18.0, 18.0)
    return values.astype(jnp.bfloat16)


def block_scale(own_key, shape, pieces, low, high):
    level, own = 1.0, jax.random.fold_in(own_key, 6)
    for position, blocks in pieces:
        steps = jnp.exp(jax.random.uniform(jax.random.fold_in(own, position), (blocks,), jnp.float32, low / len(pieces), high / len(pieces)))
        level = level * jnp.repeat(steps, shape[position] // blocks).reshape([-1 if axis == position else 1 for axis in range(len(shape))])
    return level


def split_up(count, total, limit, lean):
    portions = [(1 << 20) // math.isqrt(rank ** lean) + 1 for rank in range(2, count + 1)]
    spare, given = total - limit - (count - 1), [1] * (count - 1)
    while spare > 0:
        movable = [i for i in range(count - 1) if given[i] < limit]
        whole, left = sum([portions[i] for i in movable]), spare
        for i in movable:
            more = min(limit - given[i], max(1, left * portions[i] // whole), spare)
            given[i] = given[i] + more
            spare = spare - more
    return np.array([limit] + given)


def ragged(rng, count, total, limit, slope):
    if count == 2:
        one = jax.random.randint(rng, (), max(1, total - limit), min(limit, total - 1) + 1)
        return jnp.stack([one, total - one])
    lengths = jnp.asarray(split_up(count, total, limit, slope), jnp.int32)
    twos = (count - 1) // 2
    source_of, receiver = lengths[1:1 + 2 * twos:2], lengths[2:2 + 2 * twos:2]
    room = jnp.minimum(source_of - 1, limit - receiver)
    passed = jax.random.randint(jax.random.fold_in(rng, 1), (twos,), 0, 1 << 20) % (room + 1)
    lengths = lengths.at[1:1 + 2 * twos:2].set(source_of - passed).at[2:2 + 2 * twos:2].set(receiver + passed)
    return lengths[jax.random.permutation(jax.random.fold_in(rng, 2), count)]


def normal_values(rng, dims, deviation, bound, shards=(), held_as=jnp.bfloat16):
    entries = jax.random.normal(rng, dims, jnp.float32) * deviation
    if len(shards) > 0:
        entries = block_scale(rng, dims, shards, -0.22, 0.18) * entries
    return jnp.clip(entries, min=-bound, max=bound).astype(held_as)


def setup_inputs(seed: int = 0) -> dict:
    key_of = jax.random.split(jax.random.key(seed), 8)
    return {
        "stream": draw_stream(jax.random.fold_in(key_of[7], 71), 0),
        "doc_ids": jnp.searchsorted(jnp.cumsum(ragged(key_of[1], DOCS, TOKENS, 6 * TOK, 1)), jnp.arange(TOKENS), side="right").astype(jnp.int32),
        "norm_gain": jnp.clip(1.0 + 0.18 * jax.random.normal(key_of[2], (LAYERS, D), jnp.float32), 0.099609375, 1.8984375).astype(jnp.bfloat16),
        "proj_in": normal_values(key_of[3], (LAYERS, D, POOL), D ** -0.5, 0.09375, ((1, 4), (2, 8))),
        "mix_pool": normal_values(key_of[4], (LAYERS, GROUPS, GROUP, GROUP), GROUP ** -0.5, 0.5),
        "pool_gain": jnp.clip(1.0 + 0.18 * jax.random.normal(key_of[5], (LAYERS, POOL), jnp.float32), 0.099609375, 1.8984375).astype(jnp.bfloat16),
        "proj_out": normal_values(key_of[6], (LAYERS, POOL, D), POOL ** -0.5, 0.1875, ((1, 8), (2, 4))),
    }


epsilon = 1e-06
span_reach = 15

def span_pool(padded, labels, widths):
    kept = padded.shape[0] - span_reach
    own_label = labels[span_reach:]
    summed = jnp.zeros((kept, padded.shape[1]), jnp.float32)
    counted = jnp.zeros((kept, padded.shape[1]), jnp.float32)
    for offset in range(span_reach + 1):
        first = span_reach - offset
        member = (labels[first:first + kept] == own_label)[:, None] & (offset < widths)[None, :]
        factor = member.astype(jnp.float32)
        summed = summed + padded[first:first + kept] * factor
        counted = counted + factor
    return summed / counted - padded[span_reach:]

def reference(stream, doc_ids, norm_gain, proj_in, mix_pool, pool_gain, proj_out):
    hidden = stream
    labels = (doc_ids + 1).astype(jnp.int32)
    tags = jnp.concatenate([jnp.zeros((span_reach,), jnp.int32), labels])
    channel = jnp.arange(POOL, dtype=jnp.int32)
    widths = jnp.left_shift(jnp.int32(2), channel // GROUP % 4)
    block = D // N_TP
    for layer in range(LAYERS):
        wide = hidden.astype(jnp.float32)
        scale_rows = lax.rsqrt(lax.optimization_barrier(jnp.mean(wide * wide, axis=1)) + epsilon)
        gained = (wide * norm_gain[layer].astype(jnp.float32)[None, :]).astype(jnp.bfloat16)
        summed_in = jnp.zeros((hidden.shape[0], POOL), jnp.float32)
        for piece in range(N_TP):
            partial_value = jnp.dot(gained[:, piece * block:(piece + 1) * block], proj_in[layer, piece * block:(piece + 1) * block], preferred_element_type=jnp.float32)
            summed_in = summed_in + lax.optimization_barrier(partial_value.astype(jnp.bfloat16)).astype(jnp.float32)
        mixed_in = (summed_in * scale_rows[:, None]).astype(jnp.bfloat16)
        padded = jnp.concatenate([jnp.zeros((span_reach, POOL), jnp.float32), mixed_in.astype(jnp.float32)])
        pooled = span_pool(padded, tags, widths).astype(jnp.bfloat16)
        grouped = pooled.reshape(hidden.shape[0], GROUPS, GROUP).astype(jnp.float32)
        blended = jnp.einsum('tgc,gcd->tgd', grouped, mix_pool[layer].astype(jnp.float32)).reshape(hidden.shape[0], POOL)
        mixed = (blended * pool_gain[layer].astype(jnp.float32)[None, :]).astype(jnp.bfloat16)
        update = jnp.dot(mixed, proj_out[layer], preferred_element_type=jnp.float32)
        hidden = (wide + update).astype(jnp.bfloat16)
    return hidden
```

```python
import functools

import jax
import jax.numpy as jnp
from jax import lax
from jax.experimental import pallas as pl
from jax.experimental.pallas import tpu as pltpu
from jax.sharding import PartitionSpec as P

EPSILON = 1e-06
HALO = 16
CHUNKS = 8
LAG = 4
MESH = pl.DeviceIdType.MESH
F32, BF16 = jnp.float32, jnp.bfloat16


def mixer(sp, tp, snake, x_ref, pos_ref, gain_ref, win_ref, mix_ref, pgain_ref, wout_ref, o_ref,
          win, wout, send1, own1, recv1, sum2, recv2, mixed, zbuf, hrecv,
          sq_own, sq_in1, sq_sum, sq_in2,
          ring_s, ring_r, s1, r1, s2, r2, s3, r3, hs, hr):
    layers, model_dev, chan_dev = win_ref.shape
    tokens = x_ref.shape[0]
    rows = tokens // CHUNKS
    channels = chan_dev * sp
    half = channels // 2
    group = mix_ref.shape[-1]
    model = model_dev * tp
    row_dev = wout_ref.shape[1]
    s, t = lax.axis_index("sp"), lax.axis_index("tp")
    core = lax.rem(t, 2)
    partner = t + 1 - 2 * core
    across = lax.rem(t + 2, tp)

    def place(device):
        if not snake:
            return device
        z, y = device // 2, lax.rem(device, 2)
        return z * (1 - y) + (sp - 1 - z) * y

    def device_at(place):
        if not snake:
            return place
        up = place // (sp // 2)
        return 2 * (place * (1 - up) + (sp - 1 - place) * up) + up

    here = place(s)
    after, before = device_at(lax.rem(here + 1, sp)), device_at(lax.rem(here + sp - 1, sp))
    following, leading = lax.rem(s + 1, sp), lax.rem(s + sp - 1, sp)

    barrier = pltpu.get_barrier_semaphore()
    for peer in ({"tp": partner}, {"tp": across}, {"sp": after}, {"sp": before}, {"sp": following}, {"sp": leading}):
        pl.semaphore_signal(barrier, inc=1, device_id=peer, device_id_type=MESH)
    pl.semaphore_wait(barrier, 6)

    ahead = sp // 2
    back = sp - 1 - ahead

    def ring_view(layer, side, piece, source, own):
        if side == 0:
            part = model_dev // 2
            cut = pl.ds(piece * part, part)
            target = win.at[layer, cut, pl.ds(pl.multiple_of(source * chan_dev, chan_dev), chan_dev)]
            return (win_ref.at[layer, cut] if own else target), target
        part = row_dev // 2
        target = wout.at[layer, pl.ds(pl.multiple_of(source * row_dev + piece * part, part), part)]
        return (wout_ref.at[layer, pl.ds(piece * part, part)] if own else target), target

    def ring_copy(layer, side, piece, way, hop, own):
        origin = here - hop + sp if way == 0 else here + hop
        source = device_at(lax.rem(origin, sp))
        src, dst = ring_view(layer, side, piece, source, own)
        return pltpu.make_async_remote_copy(
            src_ref=src, dst_ref=dst,
            send_sem=ring_s.at[layer, side, piece, way, hop], recv_sem=ring_r.at[layer, side, piece, way, hop],
            device_id={"sp": after if way == 0 else before}, device_id_type=MESH)

    def ring_land(layer, side, piece, way, hop):
        origin = here - hop - 1 + 2 * sp if way == 0 else here + hop + 1
        _, dst = ring_view(layer, side, piece, device_at(lax.rem(origin, sp)), False)
        return pltpu.make_async_remote_copy(
            src_ref=dst, dst_ref=dst,
            send_sem=ring_s.at[layer, side, piece, way, hop], recv_sem=ring_r.at[layer, side, piece, way, hop],
            device_id={"sp": after if way == 0 else before}, device_id_type=MESH)

    def ring_start(layer, side, piece):
        for way in range(2):
            if (ahead, back)[way] > 0:
                ring_copy(layer, side, piece, way, 0, True).start()

    def ring_step(layer, side, piece, hop):
        for way, hops in ((0, ahead), (1, back)):
            @pl.when(hop < hops)
            def _():
                ring_land(layer, side, piece, way, hop).wait_recv()

            @pl.when(hop + 1 < hops)
            def _():
                ring_copy(layer, side, piece, way, hop + 1, False).start()

    item_count = 2 * layers
    per_step = -(-ahead // (CHUNKS // 2))
    item_steps = -(-ahead // per_step)

    def pump(step, piece):
        item = 1 + step // item_steps
        layer, side = item // 2, lax.rem(item, 2)

        @pl.when(item < item_count)
        def _():
            for which in range(2):
                @pl.when(side == which)
                def _():
                    for j in range(per_step):
                        hop = lax.rem(step, item_steps) * per_step + j
                        if ahead % per_step == 0:
                            ring_step(layer, which, piece, hop)
                        else:
                            @pl.when(hop < ahead)
                            def _():
                                ring_step(layer, which, piece, hop)

        following_item = item + 1

        @pl.when((following_item < item_count) & (lax.rem(step, item_steps) == max(item_steps - 2, 0)))
        def _():
            for which in range(2):
                @pl.when(lax.rem(following_item, 2) == which)
                def _():
                    ring_start(following_item // 2, which, piece)

    for piece in range(2):
        ring_start(0, 0, piece)
    for layer in range(layers):
        win[layer, :, pl.ds(pl.multiple_of(s * chan_dev, chan_dev), chan_dev)] = win_ref[layer]
        wout[layer, pl.ds(pl.multiple_of(s * row_dev, row_dev), row_dev), :] = wout_ref[layer]

    @pl.loop(0, CHUNKS)
    def _(i):
        at = pl.ds(pl.multiple_of(i * rows, rows), rows)
        o_ref[at] = x_ref[at]

    @pl.loop(0, ahead)
    def _(hop):
        for piece in range(2):
            ring_step(0, 0, piece, hop)
            @pl.when(hop == max(ahead - 2, 0))
            def _():
                ring_start(0, 1, piece)

    def split(step):
        layer = step // CHUNKS
        return layer, CHUNKS - 1 - lax.rem(step, CHUNKS)

    def copy1(i):
        return [pltpu.make_async_remote_copy(
            src_ref=a, dst_ref=b, send_sem=s1.at[j, i], recv_sem=r1.at[j, i],
            device_id={"tp": partner}, device_id_type=MESH)
            for j, (a, b) in enumerate(((send1.at[i], recv1.at[i]), (sq_own.at[i], sq_in1.at[i])))]

    def copy2(layer, i):
        par = lax.rem(layer, 2)
        return [pltpu.make_async_remote_copy(
            src_ref=a, dst_ref=b, send_sem=s2.at[j, i], recv_sem=r2.at[j, par, i],
            device_id={"tp": across}, device_id_type=MESH)
            for j, (a, b) in enumerate(((sum2.at[i], recv2.at[par, i]), (sq_sum.at[i], sq_in2.at[par, i])))]

    def copy3(i, side):
        view = mixed.at[i, :, pl.ds(pl.multiple_of(side * half, half), half)]
        return pltpu.make_async_remote_copy(
            src_ref=view, dst_ref=view, send_sem=s3.at[i], recv_sem=r3.at[i],
            device_id={"tp": partner}, device_id_type=MESH)

    def halo_copy(layer):
        return pltpu.make_async_remote_copy(
            src_ref=zbuf.at[pl.ds(tokens, HALO)], dst_ref=hrecv.at[layer], send_sem=hs.at[layer], recv_sem=hr.at[layer],
            device_id={"sp": following}, device_id_type=MESH)

    def project(step):
        layer, i = split(step)
        at = pl.ds(pl.multiple_of(i * rows, rows), rows)
        wide = o_ref[at].astype(F32)
        squares = wide * wide
        lanes = squares[:, :128]
        for j in range(1, model_dev // 128):
            lanes = lanes + squares[:, j * 128:(j + 1) * 128]
        sq_own[i] = jnp.sum(lanes.T.reshape(16, 8, rows), axis=0)
        gained = (wide * gain_ref[layer]).astype(BF16)
        other = pl.ds(pl.multiple_of((1 - core) * half, half), half)
        send1[i] = jnp.dot(gained, win[layer, :, other], preferred_element_type=F32).astype(BF16)
        for c in copy1(i):
            c.start()
        mine = pl.ds(pl.multiple_of(core * half, half), half)
        own1[i] = jnp.dot(gained, win[layer, :, mine], preferred_element_type=F32).astype(BF16)

    def join(step):
        layer, i = split(step)
        for c in copy1(i):
            c.wait()
        sum2[i] = (own1[i].astype(F32) + recv1[i].astype(F32)).astype(BF16)
        sq_sum[i] = sq_own[i] + sq_in1[i]
        for c in copy2(layer, i):
            c.start()

    def normalise(step):
        layer, i = split(step)
        par = lax.rem(layer, 2)
        for c in copy2(layer, i):
            c.wait()

        @pl.when(i == CHUNKS - 2)
        def _():
            halo_copy(layer).wait_send()

        total = jnp.sum(sq_sum[i] + sq_in2[par, i], axis=0, keepdims=True)
        scale = jnp.broadcast_to(lax.rsqrt(total / model + EPSILON), (128, rows)).T
        at = pl.ds(pl.multiple_of(HALO + i * rows, HALO), rows)
        for j in range(half // 128):
            cols = slice(j * 128, (j + 1) * 128)
            zbuf[at, cols] = ((sum2[i, :, cols].astype(F32) + recv2[par, i, :, cols].astype(F32)) * scale).astype(BF16)

        @pl.when(i == CHUNKS - 1)
        def _():
            halo_copy(layer).start()

    def pool(step):
        layer, i = split(step)

        @pl.when(i == 0)
        def _():
            halo_copy(layer).wait_recv()
            zbuf[pl.ds(0, HALO)] = hrecv[layer]

        wide_at = pl.ds(pl.multiple_of(i * rows, HALO), rows + HALO)
        pos = pos_ref[wide_at]
        for g in range(half // group):
            cols = slice(g * group, (g + 1) * group)
            z = zbuf[wide_at, cols].astype(F32)
            window = 2 ** (1 + g % 4)
            total = z
            step_rows = 1
            while step_rows < window:
                total = total + jnp.where(pos >= step_rows, pltpu.roll(total, step_rows, 0), 0.0)
                step_rows *= 2
            count = jnp.minimum(pos[HALO:] + 1.0, float(window))
            pooled = (total[HALO:] / count - z[HALO:]).astype(BF16)
            blended = jnp.dot(pooled, mix_ref[layer, g], preferred_element_type=F32)
            place_at = pl.ds(pl.multiple_of(core * half + g * group, group), group)
            mixed[i, :, place_at] = (blended * pgain_ref[layer, :, cols]).astype(BF16)
        copy3(i, core).start()

    def finish(step):
        layer, i = split(step)
        copy3(i, core).wait_send()
        copy3(i, 1 - core).wait_recv()
        at = pl.ds(pl.multiple_of(i * rows, rows), rows)
        for j in range(2):
            cols = slice(j * (model_dev // 2), (j + 1) * (model_dev // 2))
            update = jnp.dot(mixed[i], wout[layer, :, cols], preferred_element_type=F32)
            o_ref[at, cols] = (o_ref[at, cols].astype(F32) + update).astype(BF16)

    steps = layers * CHUNKS

    @pl.loop(0, steps + LAG)
    def _(k):
        pump(k, 0)

        @pl.when(k < steps)
        def _():
            project(k)

        pump(k, 1)

        @pl.when((k >= LAG - 1) & (k < steps + LAG - 1))
        def _():
            normalise(k - (LAG - 1))

        @pl.when(k >= LAG)
        def _():
            pool(k - LAG)

        @pl.when(k < steps)
        def _():
            join(k)

        @pl.when(k >= LAG)
        def _():
            finish(k - LAG)

    @pl.loop(0, layers)
    def _(layer):
        for side in range(2):
            for piece in range(2):
                for way, hops in ((0, ahead), (1, back)):
                    @pl.loop(0, hops)
                    def _(hop):
                        ring_copy(layer, side, piece, way, hop, False).wait_send()


def distances(doc_ids, sp):
    labels = doc_ids + 1
    reach = 2 * HALO
    earlier = lax.ppermute(labels[-reach:], "sp", [(i, i + 1) for i in range(sp - 1)])
    padded = jnp.concatenate([earlier, labels])
    kept = labels.shape[0] + HALO
    own = padded[HALO:]
    same = jnp.zeros((kept,), F32)
    for offset in range(1, HALO):
        same = same + (padded[HALO - offset:HALO - offset + kept] == own).astype(F32)
    return jnp.broadcast_to(same[:, None], (kept, 128))


def body(snake, sp, tp, stream, doc_ids, norm_gain, proj_in, mix_pool, pool_gain, proj_out):
    layers, model_dev, chan_dev = proj_in.shape
    tokens = stream.shape[0]
    rows = tokens // CHUNKS
    channels = chan_dev * sp
    half = channels // 2
    groups = mix_pool.shape[1] // 2
    t = lax.axis_index("tp")
    core = t % 2
    gain = lax.dynamic_slice_in_dim(norm_gain, t * model_dev, model_dev, 1).astype(F32)[:, None, :]
    mix = lax.dynamic_slice_in_dim(mix_pool, core * groups, groups, 1)
    pgain = lax.dynamic_slice_in_dim(pool_gain, core * half, half, 1).astype(F32)[:, None, :]
    pos = distances(doc_ids, sp)
    hops = sp // 2
    dma, vmem = pltpu.SemaphoreType.DMA, pltpu.VMEM
    return pl.pallas_call(
        functools.partial(mixer, sp, tp, snake),
        out_shape=jax.ShapeDtypeStruct(stream.shape, BF16),
        in_specs=[pl.BlockSpec(memory_space=pltpu.VMEM)] * 7,
        out_specs=pl.BlockSpec(memory_space=pltpu.VMEM),
        scratch_shapes=[
            vmem((layers, model_dev, channels), BF16),
            vmem((layers, channels, model_dev), BF16),
            vmem((CHUNKS, rows, half), BF16),
            vmem((CHUNKS, rows, half), BF16),
            vmem((CHUNKS, rows, half), BF16),
            vmem((CHUNKS, rows, half), BF16),
            vmem((2, CHUNKS, rows, half), BF16),
            vmem((CHUNKS, rows, channels), BF16),
            vmem((HALO + tokens, half), BF16),
            vmem((layers, HALO, half), BF16),
            vmem((CHUNKS, 8, rows), F32),
            vmem((CHUNKS, 8, rows), F32),
            vmem((CHUNKS, 8, rows), F32),
            vmem((2, CHUNKS, 8, rows), F32),
            dma((layers, 2, 2, 2, hops)),
            dma((layers, 2, 2, 2, hops)),
            dma((2, CHUNKS)), dma((2, CHUNKS)),
            dma((2, CHUNKS)), dma((2, 2, CHUNKS)),
            dma((CHUNKS,)), dma((CHUNKS,)),
            dma((layers,)), dma((layers,)),
        ],
        compiler_params=pltpu.CompilerParams(
            collective_id=0, has_side_effects=True, vmem_limit_bytes=60 * 2**20),
    )(stream, pos, gain, proj_in, mix, pgain, proj_out)


span_reach = 15


def shifted(value, axis, steps):
    count = lax.axis_size(axis)
    initial, last = (max(0, -steps), min(count, count - steps))
    return lax.ppermute(value, axis, [(source, source + steps) for source in range(initial, last)])


def span_pool(padded, labels, widths):
    kept = padded.shape[0] - span_reach
    own_label = labels[span_reach:]
    summed = jnp.zeros((kept, padded.shape[1]), jnp.float32)
    counted = jnp.zeros((kept, padded.shape[1]), jnp.float32)
    for offset in range(span_reach + 1):
        first = span_reach - offset
        member = (labels[first : first + kept] == own_label)[:, None] & (offset < widths)[None, :]
        factor = member.astype(jnp.float32)
        summed = summed + padded[first : first + kept] * factor
        counted = counted + factor
    return summed / counted - padded[span_reach:]


def plain_body(stream, doc_ids, norm_gain, proj_in, mix_pool, pool_gain, proj_out):
    width_dev = stream.shape[1]
    tp_count = lax.axis_size("tp")
    model_width = width_dev * tp_count
    group_size = mix_pool.shape[2]
    channels = proj_in.shape[2] * lax.axis_size("sp")
    local = channels // tp_count
    groups_dev = local // group_size
    column = lax.axis_index("tp")
    chan_ids = column * local + jnp.arange(local, dtype=jnp.int32)
    widths = jnp.left_shift(jnp.int32(2), chan_ids // group_size % 4)
    labels = (doc_ids + 1).astype(jnp.bfloat16)
    hidden_state = stream
    layer_count = proj_in.shape[0]
    in_whole, out_whole = (
        lax.all_gather(proj_in, "sp", axis=2, tiled=True),
        lax.all_gather(proj_out, "sp", axis=1, tiled=True),
    )
    for layer in range(layer_count):
        row_count = hidden_state.shape[0]
        wide = hidden_state.astype(jnp.float32)
        own_squares = jnp.sum(wide * wide, axis=1)
        gain = lax.dynamic_slice_in_dim(norm_gain[layer], column * width_dev, width_dev).astype(
            jnp.float32
        )
        gained = (wide * gain[None, :]).astype(jnp.bfloat16)
        partial_value = jnp.dot(gained, in_whole[layer], preferred_element_type=jnp.float32)
        squares = lax.psum(own_squares, "tp")
        summed_in = lax.psum_scatter(
            partial_value.astype(jnp.bfloat16), "tp", scatter_dimension=1, tiled=True
        ).astype(jnp.float32)
        row_scale = lax.rsqrt(squares / model_width + EPSILON)
        mixed_in = (summed_in * row_scale[:, None]).astype(jnp.bfloat16)
        before, before_labels = shifted((mixed_in[-span_reach:], labels[-span_reach:]), "sp", 1)
        padded = jnp.concatenate([before, mixed_in], axis=0).astype(jnp.float32)
        tags = jnp.concatenate([before_labels, labels], axis=0)
        pooled = span_pool(padded, tags, widths).astype(jnp.bfloat16)
        grouped = pooled.reshape(row_count, groups_dev, group_size)
        mixing = lax.dynamic_slice_in_dim(mix_pool[layer], column * groups_dev, groups_dev, 0)
        blended = jnp.einsum(
            "tgc,gcd->tgd", grouped, mixing, preferred_element_type=jnp.float32
        ).reshape(row_count, local)
        scale = lax.dynamic_slice_in_dim(pool_gain[layer], column * local, local).astype(
            jnp.float32
        )
        mixed = (blended * scale[None, :]).astype(jnp.bfloat16)
        full_mixed = lax.all_gather(mixed, "tp", axis=1, tiled=True)
        update = jnp.dot(full_mixed, out_whole[layer], preferred_element_type=jnp.float32)
        hidden_state = (wide + update).astype(jnp.bfloat16)
    return hidden_state


def solution(mesh):
    sp, tp = mesh.shape["sp"], mesh.shape["tp"]
    in_specs = (P("sp", "tp"), P("sp"), P(), P(None, "tp", "sp"), P(), P(), P(None, "sp", "tp"))

    def whole(stream, doc_ids, norm_gain, proj_in, mix_pool, pool_gain, proj_out):
        fits = tp == 4 and sp % 2 == 0 and proj_in.shape[2] // sp % 128 == 0 and mix_pool.shape[1] % 8 == 0
        part = functools.partial(body, True, sp, tp) if fits else plain_body
        return jax.shard_map(part, mesh=mesh, in_specs=in_specs, out_specs=P("sp", "tp"), check_vma=False)(
            stream, doc_ids, norm_gain, proj_in, mix_pool, pool_gain, proj_out)

    return whole
```

```python
import functools

import jax
import jax.numpy as jnp
from jax import lax
from jax.experimental import pallas as pl
from jax.experimental.pallas import tpu as pltpu
from jax.sharding import PartitionSpec as P

EPSILON = 1e-06
HALO = 16
CHUNKS = 8
LAG = 4
MESH = pl.DeviceIdType.MESH
F32, BF16 = jnp.float32, jnp.bfloat16


def mixer(sp, tp, snake, x_ref, doc_ref, gains_ref, win_ref, mix_ref, pgains_ref, wout_ref, o_ref,
          win, wout, send1, own1, recv1, sum2, recv2, mixed, zbuf, hrecv,
          sq_own, sq_in1, sq_sum, sq_in2,
          labels, before_labels, pos_ref, gain_ref, pgain_ref, ls, lr,
          ring_s, ring_r, s1, r1, s2, r2, s3, r3, hs, hr):
    layers, model_dev, chan_dev = win_ref.shape
    tokens = x_ref.shape[0]
    rows = tokens // CHUNKS
    channels = chan_dev * sp
    half = channels // 2
    group = mix_ref.shape[-1]
    model = model_dev * tp
    row_dev = wout_ref.shape[1]
    s, t = lax.axis_index("sp"), lax.axis_index("tp")
    core = lax.rem(t, 2)
    partner = t + 1 - 2 * core
    across = lax.rem(t + 2, tp)

    def place(device):
        if not snake:
            return device
        z, y = device // 2, lax.rem(device, 2)
        return z * (1 - y) + (sp - 1 - z) * y

    def device_at(place):
        if not snake:
            return place
        up = place // (sp // 2)
        return 2 * (place * (1 - up) + (sp - 1 - place) * up) + up

    here = place(s)
    after, before = device_at(lax.rem(here + 1, sp)), device_at(lax.rem(here + sp - 1, sp))
    following, leading = lax.rem(s + 1, sp), lax.rem(s + sp - 1, sp)

    barrier = pltpu.get_barrier_semaphore()
    for peer in ({"tp": partner}, {"tp": across}, {"sp": after}, {"sp": before}, {"sp": following}, {"sp": leading}):
        pl.semaphore_signal(barrier, inc=1, device_id=peer, device_id_type=MESH)
    pl.semaphore_wait(barrier, 6)

    ahead = sp // 2

    def hops(way, piece):
        return ahead if way == piece else ahead - 1

    def ring_view(layer, side, piece, source, own):
        if side == 0:
            part = model_dev // 2
            cut = pl.ds(piece * part, part)
            target = win.at[layer, cut, pl.ds(pl.multiple_of(source * chan_dev, chan_dev), chan_dev)]
            return (win_ref.at[layer, cut] if own else target), target
        part = row_dev // 2
        target = wout.at[layer, pl.ds(pl.multiple_of(source * row_dev + piece * part, part), part)]
        return (wout_ref.at[layer, pl.ds(piece * part, part)] if own else target), target

    def ring_copy(layer, side, piece, way, hop, own):
        origin = here - hop + sp if way == 0 else here + hop
        source = device_at(lax.rem(origin, sp))
        src, dst = ring_view(layer, side, piece, source, own)
        return pltpu.make_async_remote_copy(
            src_ref=src, dst_ref=dst,
            send_sem=ring_s.at[layer, side, piece, way, hop], recv_sem=ring_r.at[layer, side, piece, way, hop],
            device_id={"sp": after if way == 0 else before}, device_id_type=MESH)

    def ring_land(layer, side, piece, way, hop):
        origin = here - hop - 1 + 2 * sp if way == 0 else here + hop + 1
        _, dst = ring_view(layer, side, piece, device_at(lax.rem(origin, sp)), False)
        return pltpu.make_async_remote_copy(
            src_ref=dst, dst_ref=dst,
            send_sem=ring_s.at[layer, side, piece, way, hop], recv_sem=ring_r.at[layer, side, piece, way, hop],
            device_id={"sp": after if way == 0 else before}, device_id_type=MESH)

    def ring_start(layer, side, piece):
        for way in range(2):
            if hops(way, piece) > 0:
                ring_copy(layer, side, piece, way, 0, True).start()

    def ring_step(layer, side, piece, hop):
        for way in range(2):
            @pl.when(hop < hops(way, piece))
            def _():
                ring_land(layer, side, piece, way, hop).wait_recv()

            @pl.when(hop + 1 < hops(way, piece))
            def _():
                ring_copy(layer, side, piece, way, hop + 1, False).start()

    item_count = 2 * layers
    per_step = -(-ahead // (CHUNKS // 2))
    item_steps = -(-ahead // per_step)

    def pump(step, piece):
        item = 1 + step // item_steps
        layer, side = item // 2, lax.rem(item, 2)

        @pl.when(item < item_count)
        def _():
            for which in range(2):
                @pl.when(side == which)
                def _():
                    for j in range(per_step):
                        hop = lax.rem(step, item_steps) * per_step + j
                        if ahead % per_step == 0:
                            ring_step(layer, which, piece, hop)
                        else:
                            @pl.when(hop < ahead)
                            def _():
                                ring_step(layer, which, piece, hop)

        following_item = item + 1

        @pl.when((following_item < item_count) & (lax.rem(step, item_steps) == max(item_steps - 2, 0)))
        def _():
            for which in range(2):
                @pl.when(lax.rem(following_item, 2) == which)
                def _():
                    ring_start(following_item // 2, which, piece)

    for piece in range(2):
        ring_start(0, 0, piece)
    reach = 2 * HALO
    documents = doc_ref[...].astype(F32)
    for j in range(tokens // 128):
        labels[pl.ds(reach + j * 128, 128)] = jnp.broadcast_to(documents[j:j + 1], (128, 128)).T
    label_copy = pltpu.make_async_remote_copy(
        src_ref=labels.at[pl.ds(tokens, reach)], dst_ref=before_labels, send_sem=ls, recv_sem=lr,
        device_id={"sp": following}, device_id_type=MESH)
    label_copy.start()
    for layer in range(layers):
        win[layer, :, pl.ds(pl.multiple_of(s * chan_dev, chan_dev), chan_dev)] = win_ref[layer]
        wout[layer, pl.ds(pl.multiple_of(s * row_dev, row_dev), row_dev), :] = wout_ref[layer]
        own_gain = gains_ref[:, pl.ds(pl.multiple_of(t * model_dev, model_dev), model_dev)].astype(F32)
        gain_ref[layer] = own_gain[layer:layer + 1]
        own_gain = pgains_ref[:, pl.ds(pl.multiple_of(core * half, half), half)].astype(F32)
        pgain_ref[layer] = own_gain[layer:layer + 1]

    def distances(ext):
        same = jnp.zeros((ext.shape[0] - HALO, 128), F32)
        for offset in range(1, HALO):
            same = same + (pltpu.roll(ext, offset, 0) == ext)[HALO:].astype(F32)
        return same

    label_copy.wait()
    labels[pl.ds(0, reach)] = jnp.where(s == 0, -1.0, before_labels[...])
    pos_ref[pl.ds(0, HALO)] = distances(labels[pl.ds(0, reach)])

    def prepare(i):
        at = pl.ds(pl.multiple_of(i * rows, rows), rows)
        o_ref[at] = x_ref[at]
        pos_ref[pl.ds(pl.multiple_of(HALO + i * rows, HALO), rows)] = distances(
            labels[pl.ds(pl.multiple_of(HALO + i * rows, HALO), rows + HALO)])

    @pl.loop(0, ahead)
    def _(hop):
        for piece in range(2):
            ring_step(0, 0, piece, hop)
            @pl.when(hop == max(ahead - 2, 0))
            def _():
                ring_start(0, 1, piece)

        share = -(-CHUNKS // ahead)
        for j in range(share):
            @pl.when(hop * share + j < CHUNKS)
            def _():
                prepare(hop * share + j)

    def split(step):
        layer = step // CHUNKS
        return layer, CHUNKS - 1 - lax.rem(step, CHUNKS)

    def copy1(i):
        return [pltpu.make_async_remote_copy(
            src_ref=a, dst_ref=b, send_sem=s1.at[j, i], recv_sem=r1.at[j, i],
            device_id={"tp": partner}, device_id_type=MESH)
            for j, (a, b) in enumerate(((send1.at[i], recv1.at[i]), (sq_own.at[i], sq_in1.at[i])))]

    def copy2(layer, i):
        par = lax.rem(layer, 2)
        return [pltpu.make_async_remote_copy(
            src_ref=a, dst_ref=b, send_sem=s2.at[j, i], recv_sem=r2.at[j, par, i],
            device_id={"tp": across}, device_id_type=MESH)
            for j, (a, b) in enumerate(((sum2.at[i], recv2.at[par, i]), (sq_sum.at[i], sq_in2.at[par, i])))]

    def copy3(i, side):
        view = mixed.at[i, :, pl.ds(pl.multiple_of(side * half, half), half)]
        return pltpu.make_async_remote_copy(
            src_ref=view, dst_ref=view, send_sem=s3.at[i], recv_sem=r3.at[i],
            device_id={"tp": partner}, device_id_type=MESH)

    def halo_copy(layer):
        return pltpu.make_async_remote_copy(
            src_ref=zbuf.at[pl.ds(tokens, HALO)], dst_ref=hrecv.at[layer], send_sem=hs.at[layer], recv_sem=hr.at[layer],
            device_id={"sp": following}, device_id_type=MESH)

    def project(step):
        layer, i = split(step)
        at = pl.ds(pl.multiple_of(i * rows, rows), rows)
        wide = o_ref[at].astype(F32)
        squares = wide * wide
        lanes = squares[:, :128]
        for j in range(1, model_dev // 128):
            lanes = lanes + squares[:, j * 128:(j + 1) * 128]
        sq_own[i] = jnp.sum(lanes.T.reshape(16, 8, rows), axis=0)
        gained = (wide * gain_ref[layer]).astype(BF16)
        other = pl.ds(pl.multiple_of((1 - core) * half, half), half)
        send1[i] = jnp.dot(gained, win[layer, :, other], preferred_element_type=F32).astype(BF16)
        for c in copy1(i):
            c.start()
        mine = pl.ds(pl.multiple_of(core * half, half), half)
        own1[i] = jnp.dot(gained, win[layer, :, mine], preferred_element_type=F32).astype(BF16)

    def join(step):
        layer, i = split(step)
        for c in copy1(i):
            c.wait()
        sum2[i] = (own1[i].astype(F32) + recv1[i].astype(F32)).astype(BF16)
        sq_sum[i] = sq_own[i] + sq_in1[i]
        for c in copy2(layer, i):
            c.start()

    def normalise(step):
        layer, i = split(step)
        par = lax.rem(layer, 2)
        for c in copy2(layer, i):
            c.wait()

        @pl.when(i == CHUNKS - 2)
        def _():
            halo_copy(layer).wait_send()

        total = jnp.sum(sq_sum[i] + sq_in2[par, i], axis=0, keepdims=True)
        scale = jnp.broadcast_to(lax.rsqrt(total / model + EPSILON), (128, rows)).T
        at = pl.ds(pl.multiple_of(HALO + i * rows, HALO), rows)
        for j in range(half // 128):
            cols = slice(j * 128, (j + 1) * 128)
            zbuf[at, cols] = ((sum2[i, :, cols].astype(F32) + recv2[par, i, :, cols].astype(F32)) * scale).astype(BF16)

        @pl.when(i == CHUNKS - 1)
        def _():
            halo_copy(layer).start()

    def pool(step):
        layer, i = split(step)

        @pl.when(i == 0)
        def _():
            halo_copy(layer).wait_recv()
            zbuf[pl.ds(0, HALO)] = hrecv[layer]

        wide_at = pl.ds(pl.multiple_of(i * rows, HALO), rows + HALO)
        pos = pos_ref[wide_at]
        for g in range(half // group):
            cols = slice(g * group, (g + 1) * group)
            z = zbuf[wide_at, cols].astype(F32)
            window = 2 ** (1 + g % 4)
            total = z
            step_rows = 1
            while step_rows < window:
                total = total + jnp.where(pos >= step_rows, pltpu.roll(total, step_rows, 0), 0.0)
                step_rows *= 2
            count = jnp.minimum(pos[HALO:] + 1.0, float(window))
            pooled = (total[HALO:] / count - z[HALO:]).astype(BF16)
            blended = jnp.dot(pooled, mix_ref[layer, core * (half // group) + g], preferred_element_type=F32)
            place_at = pl.ds(pl.multiple_of(core * half + g * group, group), group)
            mixed[i, :, place_at] = (blended * pgain_ref[layer, :, cols]).astype(BF16)
        copy3(i, core).start()

    def finish(step):
        layer, i = split(step)
        copy3(i, core).wait_send()
        copy3(i, 1 - core).wait_recv()
        at = pl.ds(pl.multiple_of(i * rows, rows), rows)
        for j in range(2):
            cols = slice(j * (model_dev // 2), (j + 1) * (model_dev // 2))
            update = jnp.dot(mixed[i], wout[layer, :, cols], preferred_element_type=F32)
            o_ref[at, cols] = (o_ref[at, cols].astype(F32) + update).astype(BF16)

    steps = layers * CHUNKS

    @pl.loop(0, steps + LAG)
    def _(k):
        pump(k, 0)

        @pl.when(k < steps)
        def _():
            project(k)

        pump(k, 1)

        @pl.when((k >= LAG - 1) & (k < steps + LAG - 1))
        def _():
            normalise(k - (LAG - 1))

        @pl.when(k >= LAG)
        def _():
            pool(k - LAG)

        @pl.when(k < steps)
        def _():
            join(k)

        @pl.when(k >= LAG)
        def _():
            finish(k - LAG)

    @pl.loop(0, layers)
    def _(layer):
        for side in range(2):
            for piece in range(2):
                for way in range(2):
                    @pl.loop(0, hops(way, piece))
                    def _(hop):
                        ring_copy(layer, side, piece, way, hop, False).wait_send()


def body(snake, sp, tp, stream, doc_ids, norm_gain, proj_in, mix_pool, pool_gain, proj_out):
    layers, model_dev, chan_dev = proj_in.shape
    tokens = stream.shape[0]
    rows = tokens // CHUNKS
    channels = chan_dev * sp
    half = channels // 2
    hops = sp // 2
    dma, vmem = pltpu.SemaphoreType.DMA, pltpu.VMEM
    return pl.pallas_call(
        functools.partial(mixer, sp, tp, snake),
        out_shape=jax.ShapeDtypeStruct(stream.shape, BF16),
        in_specs=[pl.BlockSpec(memory_space=pltpu.VMEM)] * 7,
        out_specs=pl.BlockSpec(memory_space=pltpu.VMEM),
        scratch_shapes=[
            vmem((layers, model_dev, channels), BF16),
            vmem((layers, channels, model_dev), BF16),
            vmem((CHUNKS, rows, half), BF16),
            vmem((CHUNKS, rows, half), BF16),
            vmem((CHUNKS, rows, half), BF16),
            vmem((CHUNKS, rows, half), BF16),
            vmem((2, CHUNKS, rows, half), BF16),
            vmem((CHUNKS, rows, channels), BF16),
            vmem((HALO + tokens, half), BF16),
            vmem((layers, HALO, half), BF16),
            vmem((CHUNKS, 8, rows), F32),
            vmem((CHUNKS, 8, rows), F32),
            vmem((CHUNKS, 8, rows), F32),
            vmem((2, CHUNKS, 8, rows), F32),
            vmem((2 * HALO + tokens, 128), F32),
            vmem((2 * HALO, 128), F32),
            vmem((HALO + tokens, 128), F32),
            vmem((layers, 1, model_dev), F32),
            vmem((layers, 1, half), F32),
            dma, dma,
            dma((layers, 2, 2, 2, hops)),
            dma((layers, 2, 2, 2, hops)),
            dma((2, CHUNKS)), dma((2, CHUNKS)),
            dma((2, CHUNKS)), dma((2, 2, CHUNKS)),
            dma((CHUNKS,)), dma((CHUNKS,)),
            dma((layers,)), dma((layers,)),
        ],
        compiler_params=pltpu.CompilerParams(
            collective_id=0, has_side_effects=True, vmem_limit_bytes=60 * 2**20),
    )(stream, doc_ids.reshape(-1, 128), norm_gain, proj_in, mix_pool, pool_gain, proj_out)


span_reach = 15


def shifted(value, axis, steps):
    count = lax.axis_size(axis)
    initial, last = (max(0, -steps), min(count, count - steps))
    return lax.ppermute(value, axis, [(source, source + steps) for source in range(initial, last)])


def span_pool(padded, labels, widths):
    kept = padded.shape[0] - span_reach
    own_label = labels[span_reach:]
    summed = jnp.zeros((kept, padded.shape[1]), jnp.float32)
    counted = jnp.zeros((kept, padded.shape[1]), jnp.float32)
    for offset in range(span_reach + 1):
        first = span_reach - offset
        member = (labels[first : first + kept] == own_label)[:, None] & (offset < widths)[None, :]
        factor = member.astype(jnp.float32)
        summed = summed + padded[first : first + kept] * factor
        counted = counted + factor
    return summed / counted - padded[span_reach:]


def plain_body(stream, doc_ids, norm_gain, proj_in, mix_pool, pool_gain, proj_out):
    width_dev = stream.shape[1]
    tp_count = lax.axis_size("tp")
    model_width = width_dev * tp_count
    group_size = mix_pool.shape[2]
    channels = proj_in.shape[2] * lax.axis_size("sp")
    local = channels // tp_count
    groups_dev = local // group_size
    column = lax.axis_index("tp")
    chan_ids = column * local + jnp.arange(local, dtype=jnp.int32)
    widths = jnp.left_shift(jnp.int32(2), chan_ids // group_size % 4)
    labels = (doc_ids + 1).astype(jnp.bfloat16)
    hidden_state = stream
    layer_count = proj_in.shape[0]
    in_whole, out_whole = (
        lax.all_gather(proj_in, "sp", axis=2, tiled=True),
        lax.all_gather(proj_out, "sp", axis=1, tiled=True),
    )
    for layer in range(layer_count):
        row_count = hidden_state.shape[0]
        wide = hidden_state.astype(jnp.float32)
        own_squares = jnp.sum(wide * wide, axis=1)
        gain = lax.dynamic_slice_in_dim(norm_gain[layer], column * width_dev, width_dev).astype(
            jnp.float32
        )
        gained = (wide * gain[None, :]).astype(jnp.bfloat16)
        partial_value = jnp.dot(gained, in_whole[layer], preferred_element_type=jnp.float32)
        squares = lax.psum(own_squares, "tp")
        summed_in = lax.psum_scatter(
            partial_value.astype(jnp.bfloat16), "tp", scatter_dimension=1, tiled=True
        ).astype(jnp.float32)
        row_scale = lax.rsqrt(squares / model_width + EPSILON)
        mixed_in = (summed_in * row_scale[:, None]).astype(jnp.bfloat16)
        before, before_labels = shifted((mixed_in[-span_reach:], labels[-span_reach:]), "sp", 1)
        padded = jnp.concatenate([before, mixed_in], axis=0).astype(jnp.float32)
        tags = jnp.concatenate([before_labels, labels], axis=0)
        pooled = span_pool(padded, tags, widths).astype(jnp.bfloat16)
        grouped = pooled.reshape(row_count, groups_dev, group_size)
        mixing = lax.dynamic_slice_in_dim(mix_pool[layer], column * groups_dev, groups_dev, 0)
        blended = jnp.einsum(
            "tgc,gcd->tgd", grouped, mixing, preferred_element_type=jnp.float32
        ).reshape(row_count, local)
        scale = lax.dynamic_slice_in_dim(pool_gain[layer], column * local, local).astype(
            jnp.float32
        )
        mixed = (blended * scale[None, :]).astype(jnp.bfloat16)
        full_mixed = lax.all_gather(mixed, "tp", axis=1, tiled=True)
        update = jnp.dot(full_mixed, out_whole[layer], preferred_element_type=jnp.float32)
        hidden_state = (wide + update).astype(jnp.bfloat16)
    return hidden_state


def solution(mesh):
    sp, tp = mesh.shape["sp"], mesh.shape["tp"]
    in_specs = (P("sp", "tp"), P("sp"), P(), P(None, "tp", "sp"), P(), P(), P(None, "sp", "tp"))

    def whole(stream, doc_ids, norm_gain, proj_in, mix_pool, pool_gain, proj_out):
        fits = tp == 4 and sp % 2 == 0 and proj_in.shape[2] // sp % 128 == 0 and mix_pool.shape[1] % 8 == 0
        part = functools.partial(body, True, sp, tp) if fits else plain_body
        return jax.shard_map(part, mesh=mesh, in_specs=in_specs, out_specs=P("sp", "tp"), check_vma=False)(
            stream, doc_ids, norm_gain, proj_in, mix_pool, pool_gain, proj_out)

    return whole
```
